32 devices in a mesh: sp: 8 (over z, x), tp: 4 (over y, core).
Axes of the slice: x: 2, y: 2, z: 4, core: 2. Of those that a mesh axis runs over, the one named last changes fastest.
Arguments:
- tokens: bfloat16 [1024, 2048], P('sp'), may hold values from -6 to 6
- norm_gain: float32 [2048], replicated, may hold values from 0.1 to 1.9
- cotangent: bfloat16 [1024, 2048], P('sp'), may hold values from -8 to 8
- routes: int32 [1024, 2], P('sp'), may hold values from 0 to 3, all different within a row; in each aligned block of 128 rows (0 to 127, 128 to 255, ...) at most 128 rows name the same one
- route_weight: float32 [1024, 2], P('sp'), may hold values from 0.2 to 1
- gate_weight: bfloat16 [8, 2048, 1792], P('sp', None, 'tp'), may hold values from -0.125 to 0.125
- up_weight: bfloat16 [8, 2048, 1792], P('sp', None, 'tp'), may hold values from -0.125 to 0.125
- down_weight: bfloat16 [8, 1792, 2048], P('sp', 'tp'), may hold values from -0.09375 to 0.09375
- scan_input: bfloat16 [1024, 1024], P('sp', 'tp'), may hold values from -6 to 6
- out_gate: bfloat16 [1024, 1024], P('sp', 'tp'), may hold values from -6 to 6
- step_size: float32 [16, 1024], P('tp', 'sp'), may hold values from 0.24 to 4.1
- decay_rate: float32 [16], P('tp'), may hold values from 9.667969e-06 to 0.031
- write_keys: bfloat16 [1024, 256], P('sp', 'tp'), may hold values from -0.75 to 0.75
- read_keys: bfloat16 [1024, 256], P('sp', 'tp'), may hold values from -0.75 to 0.75
- start_state: float32 [8, 16, 64, 64], P('sp', 'tp'), may hold values from -12 to 12
- out_proj: bfloat16 [2048, 1024], P(None, 'tp'), may hold values from -0.1875 to 0.1875
Outputs:
- residual_grad: bfloat16 [1024, 2048], P('sp', 'tp')
- gate_weight_grad: bfloat16 [8, 2048, 1792], P('sp', None, 'tp')
- up_weight_grad: bfloat16 [8, 2048, 1792], P('sp', None, 'tp')
- down_weight_grad: bfloat16 [8, 1792, 2048], P('sp', 'tp')
- out_proj_grad: float32 [2048, 1024], P('sp', 'tp')
- scan_input_grad: bfloat16 [1024, 1024], P('sp', 'tp')
- out_gate_grad: bfloat16 [1024, 1024], P('sp', 'tp')
- write_keys_grad: bfloat16 [1024, 256], P('sp', 'tp')
- read_keys_grad: bfloat16 [1024, 256], P('sp', 'tp')
The draws below stay inside these ranges and needn't reach their ends.
Inputs may be any that keep to these rules, and one draw needn't show every extreme that they name: Each token names two different experts. Among the tokens of one block of 128 positions at most 128 routes name one expert, and in every draw some expert gets exactly 128 routes from some block.
All inputs are finite; a program needn't handle non-finite values.
Results may differ from the reference program's by a relative error of at most 0.0078.
Values may be sent and summed in bfloat16 or wider, within the bound.
No kernel may reach another device: no remote copies, remote signals or barrier semaphores. Data moves between devices by JAX's collectives and lax.ppermute only.
A program may use at most 128 MiB of HBM per device.

```python
import math
import jax
import jax.numpy as jnp
import numpy as np
from jax import lax

D = 2048
FF = 3584
FF_HALF = 1792
HEADS = 16
HEAD_DIM = 64
STATE = 64
GROUPS = 4
MIX = 1024
TOK_DEV = 128
BLOCKS = 8
TOKENS = 1024
EXPERTS = 4
CAP = 128
N_SP = 8


def draw_step_size(key, part):
    token_key, block_key = jax.random.split(jax.random.fold_in(key, 11))
    block_count = TOKENS // TOK_DEV
    local = jax.random.uniform(token_key, (HEADS, TOKENS), jnp.float32, -0.7, 0.7)
    slow = jax.random.uniform(block_key, (HEADS, block_count, 1), jnp.float32, -0.7, 0.7)
    slow = jnp.broadcast_to(slow, (HEADS, block_count, TOK_DEV)).reshape(HEADS, TOKENS)
    return jnp.exp(local + slow)


def draw_decay_rate(key, part):
    lowest = math.log(0.01 / TOKENS)
    highest = math.log(0.03)
    drawn = jax.random.uniform(jax.random.fold_in(key, 23), (HEADS,), jnp.float32, lowest, highest)
    return jnp.exp(drawn)


def spiked(array, key, source, target, shards_of, factor):
    owner, partner = [(jnp.arange(array.shape[dim]) // (array.shape[dim] // shards_of)).reshape([-1 if axis == dim else 1 for axis in range(array.ndim)]) for dim in (source, target)]
    chosen = jax.random.permutation(key, shards_of)[partner]
    strong = (owner == chosen) | (owner == (partner + shards_of // 2) % shards_of)
    return jnp.where(strong, factor * array, array)


def block_scale(own_key, shape, cuts, smallest, top_value):
    factor_of, own = 1.0, jax.random.fold_in(own_key, 6)
    for axis_at, blocks in cuts:
        heights = jnp.exp(jax.random.uniform(jax.random.fold_in(own, axis_at), (blocks,), jnp.float32, smallest / len(cuts), top_value / len(cuts)))
        factor_of = factor_of * jnp.repeat(heights, shape[axis_at] // blocks).reshape([-1 if axis == axis_at else 1 for axis in range(len(shape))])
    return factor_of


def deal_out(key, own, number, rows, number_of, top, reach, slope):
    order = jax.random.permutation(key, number_of)
    heavy_load, usual = load_shares(number_of, rows * top, reach, slope, True), load_shares(number_of, rows * top, reach, slope, False)
    places = jnp.arange(number_of)

    def named(sizes, turn):
        used = int((sizes > 0).sum())
        fixed = max(1, used // 4)
        shifted = fixed + (places - fixed + turn * (used - fixed)) % max(1, number_of - fixed)
        return jnp.zeros((number_of,), jnp.int32).at[order[jnp.where(places < fixed, places, shifted)]].set(jnp.asarray(sizes, jnp.int32))

    sizes = jnp.where(number % 4 == 0, named(heavy_load, number // 4), named(usual, number - number // 4 - 1))
    mixed = jax.random.permutation(jax.random.fold_in(own, 3), number_of)
    donor, sink = mixed[0:number_of // 2 * 2:2], mixed[1:number_of // 2 * 2:2]
    margin = jnp.minimum(sizes[donor] - 1, reach - sizes[sink]) // 2
    margin = jnp.where((donor == order[0]) | (sink == order[0]) | (sizes[sink] == 0), 0, jnp.maximum(margin, 0))
    shifted = jax.random.randint(jax.random.fold_in(own, 4), (number_of // 2,), 0, 1 << 20) % (margin + 1)
    sizes = sizes.at[donor].add(-shifted).at[sink].add(shifted)
    members = jnp.searchsorted(jnp.cumsum(sizes), jnp.arange(rows * top), side="right").astype(jnp.int32)
    listing = members.reshape(top, rows).T
    listing = listing[jax.random.permutation(jax.random.fold_in(own, 1), rows)]
    turn = jax.random.randint(jax.random.fold_in(own, 2), (rows, 1), 0, top)
    return jnp.take_along_axis(listing, (jnp.arange(top)[None, :] + turn) % top, axis=1)


def load_shares(count, total, reach, slope, full):
    loads = [(1 << 20) // math.isqrt(rank ** slope) + 1 for rank in range(1, count + 1)]
    largest = reach if full else min(reach, max(-(-total // count), total * loads[0] // sum(loads)))
    least = 1 if total - largest >= count - 1 else 0
    counts, surplus = [largest] + [least] * (count - 1), total - largest - least * (count - 1)
    while surplus > 0:
        free = [i for i in range(1, count) if counts[i] < largest] or [i for i in range(1, count) if counts[i] < reach]
        whole, budget = sum([loads[i] for i in free]), surplus
        for i in free:
            more = min(reach - counts[i], max(1, budget * loads[i] // whole), surplus)
            counts[i] = counts[i] + more
            surplus = surplus - more
    return np.array(counts)


def centred(stream_key, extent, scale, bound, cuts=(), kind=jnp.bfloat16):
    result = scale * jax.random.normal(stream_key, extent, jnp.float32)
    if cuts:
        result = result * block_scale(stream_key, extent, cuts, -0.22, 0.18)
    return jnp.clip(result, -bound, bound).astype(kind)


def noise_with(stream_key, shape, scale, reach, shards, heavy, dtype=jnp.bfloat16):
    values = scale * jax.random.normal(stream_key, shape, jnp.float32)
    if shards:
        values = values * block_scale(stream_key, shape, shards, -0.22, 0.18)
    return jnp.clip(spiked(values, jax.random.fold_in(stream_key, 3), *heavy), -reach, reach).astype(dtype)


def setup_inputs(seed: int = 0) -> dict:
    streams_of = jax.random.split(jax.random.key(seed), 17)
    tokens = centred(streams_of[0], (TOKENS, D), 1.0, 6.0, ((0, 8),))
    norm_gain = jnp.clip(1.0 + 0.18 * jax.random.normal(streams_of[1], (D,), jnp.float32), 0.1, 1.9)
    cotangent = noise_with(streams_of[2], (TOKENS, D), 1.0, 8.0, ((0, 8),), (0, 1, 8, 2.0))
    routes_keys = jax.random.split(jax.random.fold_in(streams_of[3], 1), TOKENS // TOK_DEV)
    routes_turns = jax.random.permutation(jax.random.fold_in(streams_of[3], 3), TOKENS // TOK_DEV)
    routes = jax.vmap(lambda own, number: deal_out(jax.random.fold_in(streams_of[3], 2), own, number, TOK_DEV, EXPERTS, 2, CAP, 1))(routes_keys, routes_turns).reshape((TOKENS, 2))
    route_weight = jnp.clip(0.2 + 0.8 * jax.random.uniform(streams_of[4], (TOKENS, 2), jnp.float32) ** block_scale(streams_of[4], (TOKENS, 2), ((0, 8),), -0.2, 0.2), 0.2, 1.0)
    gate_weight = centred(streams_of[5], (N_SP, D, FF_HALF), D ** -0.5, 0.125, ((0, 8), (2, 4)))
    up_weight = centred(streams_of[6], (N_SP, D, FF_HALF), D ** -0.5, 0.125, ((0, 8), (2, 4)))
    down_weight = centred(streams_of[7], (N_SP, FF_HALF, D), FF ** -0.5, 0.09375, ((0, 8), (1, 4)))
    scan_input = centred(streams_of[8], (TOKENS, MIX), 1.0, 6.0, ((0, 8), (1, 4)))
    out_gate = centred(streams_of[9], (TOKENS, MIX), 1.0, 6.0, ((0, 8), (1, 4)))
    step_size = draw_step_size(jax.random.fold_in(streams_of[16], 71), 0)
    decay_rate = draw_decay_rate(jax.random.fold_in(streams_of[16], 71), 0)
    write_keys = centred(streams_of[12], (TOKENS, GROUPS * STATE), 0.125, 0.75, ((0, 8), (1, 4)))
    read_keys = centred(streams_of[13], (TOKENS, GROUPS * STATE), 0.125, 0.75, ((0, 8), (1, 4)))
    start_state = centred(streams_of[14], (BLOCKS, HEADS, HEAD_DIM, STATE), 2.0, 12.0, ((0, 8), (1, 4)), jnp.float32)
    out_proj = centred(streams_of[15], (D, MIX), MIX ** -0.5, 0.1875, ((1, 4),))
    return dict(tokens=tokens, norm_gain=norm_gain, cotangent=cotangent, routes=routes, route_weight=route_weight, gate_weight=gate_weight, up_weight=up_weight, down_weight=down_weight, scan_input=scan_input, out_gate=out_gate, step_size=step_size, decay_rate=decay_rate, write_keys=write_keys, read_keys=read_keys, start_state=start_state, out_proj=out_proj)


EPS = 1e-06
HIGHEST = lax.Precision.HIGHEST

def prepare(scan_rows, step_rows, write_rows, read_rows, decay_rates, per_group):
    length = scan_rows.shape[0]
    head_count = step_rows.shape[0]
    logdec = jnp.cumsum(-decay_rates[:, None] * step_rows, axis=1)
    causal = jnp.arange(length)[:, None] >= jnp.arange(length)[None, :]
    spread = jnp.where(causal[None, :, :], logdec[:, :, None] - logdec[:, None, :], -jnp.inf)
    weights = jnp.exp(spread)
    inputs = scan_rows.astype(jnp.float32).reshape(length, head_count, -1) * jnp.transpose(step_rows)[:, :, None]
    write_head = jnp.repeat(write_rows.astype(jnp.float32).reshape(length, -1, STATE), per_group, axis=1)
    read_head = jnp.repeat(read_rows.astype(jnp.float32).reshape(length, -1, STATE), per_group, axis=1)
    scores = jnp.einsum('thn,shn->hts', read_head, write_head, precision=HIGHEST) * weights
    return (logdec, weights, inputs, write_head, read_head, scores)

def block_forward(scan_rows, gate_rows, step_rows, write_rows, read_rows, decay_rates, entry_state, mix_grad, per_group):
    logdec, weights, inputs, write_head, read_head, scores = prepare(scan_rows, step_rows, write_rows, read_rows, decay_rates, per_group)
    length, head_count = (inputs.shape[0], inputs.shape[1])
    growth = jnp.transpose(jnp.exp(logdec))
    output = jnp.einsum('hts,shp->thp', scores, inputs, precision=HIGHEST)
    output = output + growth[:, :, None] * jnp.einsum('thn,hpn->thp', read_head, entry_state, precision=HIGHEST)
    gate_val = gate_rows.astype(jnp.float32).reshape(length, head_count, -1)
    sigmoid_val = jax.nn.sigmoid(gate_val)
    gated = (output * gate_val * sigmoid_val).reshape(length, -1).astype(jnp.bfloat16)
    out_grad = mix_grad.reshape(length, head_count, -1)
    state_grad = out_grad * gate_val * sigmoid_val
    gate_grad = (out_grad * output * sigmoid_val * (1.0 + gate_val * (1.0 - sigmoid_val))).reshape(length, -1).astype(jnp.bfloat16)
    carried = jnp.einsum('th,thp,thn->hpn', growth, state_grad, read_head, precision=HIGHEST)
    return (gated, gate_grad, jnp.exp(logdec[:, -1]), carried, state_grad)

def block_back(scan_rows, step_rows, write_rows, read_rows, decay_rates, entry_state, state_grad, later_state, per_group):
    logdec, weights, inputs, write_head, read_head, scores = prepare(scan_rows, step_rows, write_rows, read_rows, decay_rates, per_group)
    length, head_count = (inputs.shape[0], inputs.shape[1])
    growth = jnp.transpose(jnp.exp(logdec))
    shrink = jnp.transpose(jnp.exp(logdec[:, -1:] - logdec))
    in_grad = jnp.einsum('hts,thp->shp', scores, state_grad, precision=HIGHEST)
    in_grad = in_grad + shrink[:, :, None] * jnp.einsum('shn,hpn->shp', write_head, later_state, precision=HIGHEST)
    scan_grad = (in_grad * jnp.transpose(step_rows)[:, :, None]).reshape(length, -1).astype(jnp.bfloat16)
    pair_terms = jnp.einsum('thp,shp->hts', state_grad, inputs, precision=HIGHEST) * weights
    read_grad = jnp.einsum('hts,shn->thn', pair_terms, write_head, precision=HIGHEST)
    read_grad = read_grad + growth[:, :, None] * jnp.einsum('thp,hpn->thn', state_grad, entry_state, precision=HIGHEST)
    write_grad = jnp.einsum('hts,thn->shn', pair_terms, read_head, precision=HIGHEST)
    write_grad = write_grad + shrink[:, :, None] * jnp.einsum('shp,hpn->shn', inputs, later_state, precision=HIGHEST)
    group_count = head_count // per_group
    read_total = lax.optimization_barrier(jnp.sum(read_grad.reshape(length, group_count, per_group, -1), axis=2)).reshape(length, -1).astype(jnp.bfloat16)
    write_total = lax.optimization_barrier(jnp.sum(write_grad.reshape(length, group_count, per_group, -1), axis=2)).reshape(length, -1).astype(jnp.bfloat16)
    return (scan_grad, write_total, read_total)

def expert_grads(rows_in, rows_cot, gate_mat, up_mat, down_mat):
    contract_rows = (((0,), (0,)), ((), ()))
    contract_cols = (((1,), (1,)), ((), ()))
    gate_pre = jnp.dot(rows_in, gate_mat, preferred_element_type=jnp.float32)
    up_pre = jnp.dot(rows_in, up_mat, preferred_element_type=jnp.float32)
    sigmoid_val = jax.nn.sigmoid(gate_pre)
    active = (gate_pre * sigmoid_val * up_pre).astype(jnp.bfloat16)
    down_grad = lax.dot_general(active, rows_cot, contract_rows, preferred_element_type=jnp.float32)
    act_grad = lax.dot_general(rows_cot, down_mat, contract_cols, preferred_element_type=jnp.float32)
    gate_pre_grad = (act_grad * up_pre * sigmoid_val * (1.0 + gate_pre * (1.0 - sigmoid_val))).astype(jnp.bfloat16)
    up_pre_grad = (act_grad * gate_pre * sigmoid_val).astype(jnp.bfloat16)
    gate_grad = lax.dot_general(rows_in, gate_pre_grad, contract_rows, preferred_element_type=jnp.float32)
    up_grad = lax.dot_general(rows_in, up_pre_grad, contract_rows, preferred_element_type=jnp.float32)
    input_grad = lax.dot_general(gate_pre_grad, gate_mat, contract_cols, preferred_element_type=jnp.float32)
    input_grad = input_grad + lax.dot_general(up_pre_grad, up_mat, contract_cols, preferred_element_type=jnp.float32)
    return (gate_grad, up_grad, down_grad, input_grad)

def reference(tokens, norm_gain, cotangent, routes, route_weight, gate_weight, up_weight, down_weight, scan_input, out_gate, step_size, decay_rate, write_keys, read_keys, start_state, out_proj):
    hidden = tokens.astype(jnp.float32)
    inverse = lax.rsqrt(lax.optimization_barrier(jnp.mean(hidden * hidden, axis=1)) + EPS)
    normed = (hidden * inverse[:, None] * norm_gain[None, :]).astype(jnp.bfloat16)
    most_rows = N_SP * CAP
    gate_whole = jnp.transpose(gate_weight.reshape(EXPERTS, 2, D, FF_HALF), (0, 2, 1, 3)).reshape(EXPERTS, D, FF)
    up_whole = jnp.transpose(up_weight.reshape(EXPERTS, 2, D, FF_HALF), (0, 2, 1, 3)).reshape(EXPERTS, D, FF)
    down_whole = down_weight.reshape(EXPERTS, FF, D)

    def expert_step(running, operands):
        expert_index, gate_mat, up_mat, down_mat = operands
        chosen = routes == expert_index
        scaling = lax.optimization_barrier(jnp.sum(jnp.where(chosen, route_weight, 0.0), axis=1))
        picked = jnp.any(chosen, axis=1)
        row_ids = jnp.nonzero(picked, size=most_rows, fill_value=0)[0]
        filled = jnp.arange(most_rows) < jnp.sum(picked.astype(jnp.int32))
        rows_in = normed[row_ids]
        scaled = (scaling[row_ids][:, None] * cotangent[row_ids].astype(jnp.float32)).astype(jnp.bfloat16)
        rows_cot = jnp.where(filled[:, None], scaled, jnp.zeros((), jnp.bfloat16))
        gate_grad, up_grad, down_grad, input_grad = expert_grads(rows_in, rows_cot, gate_mat, up_mat, down_mat)
        running = running.at[row_ids].add(jnp.where(filled[:, None], input_grad, 0.0))
        return (running, (gate_grad.astype(jnp.bfloat16), up_grad.astype(jnp.bfloat16), down_grad.astype(jnp.bfloat16)))
    normed_grad, (gate_all, up_all, down_all) = lax.scan(expert_step, jnp.zeros((TOKENS, D), jnp.float32), (jnp.arange(EXPERTS).astype(jnp.int32), gate_whole, up_whole, down_whole))
    gate_weight_grad = jnp.transpose(gate_all.reshape(EXPERTS, D, 2, FF_HALF), (0, 2, 1, 3)).reshape(N_SP, D, FF_HALF)
    up_weight_grad = jnp.transpose(up_all.reshape(EXPERTS, D, 2, FF_HALF), (0, 2, 1, 3)).reshape(N_SP, D, FF_HALF)
    down_weight_grad = down_all.reshape(N_SP, FF_HALF, D)
    gained = norm_gain[None, :] * normed_grad
    dotted = lax.optimization_barrier(jnp.sum(hidden * gained, axis=1))
    residual = cotangent.astype(jnp.float32) + inverse[:, None] * gained - hidden * (inverse ** 3 * dotted / D)[:, None]
    residual_grad = residual.astype(jnp.bfloat16)
    mix_grad = jnp.dot(residual_grad, out_proj, preferred_element_type=jnp.float32)
    per_group = HEADS // GROUPS
    scan_blocks = scan_input.reshape(BLOCKS, TOK_DEV, MIX)
    gate_blocks = out_gate.reshape(BLOCKS, TOK_DEV, MIX)
    step_blocks = jnp.transpose(step_size.reshape(HEADS, BLOCKS, TOK_DEV), (1, 0, 2))
    write_blocks = write_keys.reshape(BLOCKS, TOK_DEV, GROUPS * STATE)
    read_blocks = read_keys.reshape(BLOCKS, TOK_DEV, GROUPS * STATE)
    mix_blocks = mix_grad.reshape(BLOCKS, TOK_DEV, MIX)

    def forward_one(operands):
        scan_rows, gate_rows, step_rows, write_rows, read_rows, entry_state, mix_rows = operands
        return block_forward(scan_rows, gate_rows, step_rows, write_rows, read_rows, decay_rate, entry_state, mix_rows, per_group)
    gated, gate_grads, decays, carries, state_grads = lax.map(forward_one, (scan_blocks, gate_blocks, step_blocks, write_blocks, read_blocks, start_state, mix_blocks))

    def back_step(later_state, operands):
        decay_now, carry_now = operands
        return (carry_now + decay_now[:, None, None] * later_state, later_state)
    _, later_all = lax.scan(back_step, jnp.zeros((HEADS, HEAD_DIM, STATE), jnp.float32), (decays, carries), reverse=True)

    def back_one(operands):
        scan_rows, step_rows, write_rows, read_rows, entry_state, state_grad, later_state = operands
        return block_back(scan_rows, step_rows, write_rows, read_rows, decay_rate, entry_state, state_grad, later_state, per_group)
    scan_grads, write_grads, read_grads = lax.map(back_one, (scan_blocks, step_blocks, write_blocks, read_blocks, start_state, state_grads, later_all))
    gated_all = gated.reshape(TOKENS, MIX)
    out_proj_grad = jnp.dot(jnp.transpose(residual_grad), gated_all, preferred_element_type=jnp.float32)
    return (residual_grad, gate_weight_grad, up_weight_grad, down_weight_grad, out_proj_grad, scan_grads.reshape(TOKENS, MIX), gate_grads.reshape(TOKENS, MIX), write_grads.reshape(TOKENS, GROUPS * STATE), read_grads.reshape(TOKENS, GROUPS * STATE))
```

```python
import jax
import jax.numpy as jnp
from jax import lax
from jax.sharding import PartitionSpec as P

D = 2048
HEADS = 16
STATE = 64
GROUPS = 4


EPS = 1e-06
HIGHEST = lax.Precision.HIGHEST


def swapped(value, axis, apart):
    mask = 2**apart
    pairs = [(source, source ^ mask) for source in range(lax.axis_size(axis))]
    return lax.ppermute(value, axis, pairs)


def prefix(part, axis, combine, identity):
    count = lax.axis_size(axis)
    place = lax.axis_index(axis)
    ahead = count - 1 - place
    gathered = jax.tree.map(lambda a: lax.all_gather(a, axis), part)
    state = jax.tree.map(lambda a, e: jnp.zeros_like(a) + jnp.asarray(e, a.dtype), part, identity)

    def one(hop, state):
        source = count - 1 - hop
        return combine(
            state, jax.tree.map(lambda a: lax.dynamic_index_in_dim(a, source, 0, False), gathered)
        )

    return lax.fori_loop(0, ahead, one, state)


def prepare(scan_rows, step_rows, write_rows, read_rows, decay_rates, per_group):
    length = scan_rows.shape[0]
    head_count = step_rows.shape[0]
    logdec = jnp.cumsum(-decay_rates[:, None] * step_rows, axis=1)
    causal = jnp.arange(length)[:, None] >= jnp.arange(length)[None, :]
    spread = jnp.where(causal[None, :, :], logdec[:, :, None] - logdec[:, None, :], -jnp.inf)
    weights = jnp.exp(spread)
    inputs = (
        scan_rows.astype(jnp.float32).reshape(length, head_count, -1)
        * jnp.transpose(step_rows)[:, :, None]
    )
    write_head = jnp.repeat(
        write_rows.astype(jnp.float32).reshape(length, -1, STATE), per_group, axis=1
    )
    read_head = jnp.repeat(
        read_rows.astype(jnp.float32).reshape(length, -1, STATE), per_group, axis=1
    )
    scores = jnp.einsum("thn,shn->hts", read_head, write_head, precision=HIGHEST) * weights
    return (logdec, weights, inputs, write_head, read_head, scores)


def block_forward(
    scan_rows,
    gate_rows,
    step_rows,
    write_rows,
    read_rows,
    decay_rates,
    entry_state,
    mix_grad,
    per_group,
):
    logdec, weights, inputs, write_head, read_head, scores = prepare(
        scan_rows, step_rows, write_rows, read_rows, decay_rates, per_group
    )
    length, head_count = (inputs.shape[0], inputs.shape[1])
    growth = jnp.transpose(jnp.exp(logdec))
    output = jnp.einsum("hts,shp->thp", scores, inputs, precision=HIGHEST)
    output = output + growth[:, :, None] * jnp.einsum(
        "thn,hpn->thp", read_head, entry_state, precision=HIGHEST
    )
    gate_val = gate_rows.astype(jnp.float32).reshape(length, head_count, -1)
    sigmoid_val = jax.nn.sigmoid(gate_val)
    gated = (output * gate_val * sigmoid_val).reshape(length, -1).astype(jnp.bfloat16)
    out_grad = mix_grad.reshape(length, head_count, -1)
    state_grad = out_grad * gate_val * sigmoid_val
    gate_grad = (
        (out_grad * output * sigmoid_val * (1.0 + gate_val * (1.0 - sigmoid_val)))
        .reshape(length, -1)
        .astype(jnp.bfloat16)
    )
    carried = jnp.einsum("th,thp,thn->hpn", growth, state_grad, read_head, precision=HIGHEST)
    return (gated, gate_grad, jnp.exp(logdec[:, -1]), carried, state_grad)


def block_back(
    scan_rows,
    step_rows,
    write_rows,
    read_rows,
    decay_rates,
    entry_state,
    state_grad,
    later_state,
    per_group,
):
    logdec, weights, inputs, write_head, read_head, scores = prepare(
        scan_rows, step_rows, write_rows, read_rows, decay_rates, per_group
    )
    length, head_count = (inputs.shape[0], inputs.shape[1])
    growth = jnp.transpose(jnp.exp(logdec))
    shrink = jnp.transpose(jnp.exp(logdec[:, -1:] - logdec))
    in_grad = jnp.einsum("hts,thp->shp", scores, state_grad, precision=HIGHEST)
    in_grad = in_grad + shrink[:, :, None] * jnp.einsum(
        "shn,hpn->shp", write_head, later_state, precision=HIGHEST
    )
    scan_grad = (
        (in_grad * jnp.transpose(step_rows)[:, :, None]).reshape(length, -1).astype(jnp.bfloat16)
    )
    pair_terms = jnp.einsum("thp,shp->hts", state_grad, inputs, precision=HIGHEST) * weights
    read_grad = jnp.einsum("hts,shn->thn", pair_terms, write_head, precision=HIGHEST)
    read_grad = read_grad + growth[:, :, None] * jnp.einsum(
        "thp,hpn->thn", state_grad, entry_state, precision=HIGHEST
    )
    write_grad = jnp.einsum("hts,thn->shn", pair_terms, read_head, precision=HIGHEST)
    write_grad = write_grad + shrink[:, :, None] * jnp.einsum(
        "shp,hpn->shn", inputs, later_state, precision=HIGHEST
    )
    group_count = head_count // per_group
    read_total = (
        jnp.sum(read_grad.reshape(length, group_count, per_group, -1), axis=2)
        .reshape(length, -1)
        .astype(jnp.bfloat16)
    )
    write_total = (
        jnp.sum(write_grad.reshape(length, group_count, per_group, -1), axis=2)
        .reshape(length, -1)
        .astype(jnp.bfloat16)
    )
    return (scan_grad, write_total, read_total)


def expert_grads(rows_in, rows_cot, gate_mat, up_mat, down_mat):
    contract_rows = (((0,), (0,)), ((), ()))
    contract_cols = (((1,), (1,)), ((), ()))
    gate_pre = jnp.dot(rows_in, gate_mat, preferred_element_type=jnp.float32)
    up_pre = jnp.dot(rows_in, up_mat, preferred_element_type=jnp.float32)
    sigmoid_val = jax.nn.sigmoid(gate_pre)
    active = (gate_pre * sigmoid_val * up_pre).astype(jnp.bfloat16)
    down_grad = lax.dot_general(active, rows_cot, contract_rows, preferred_element_type=jnp.float32)
    act_grad = lax.dot_general(
        rows_cot, down_mat, contract_cols, preferred_element_type=jnp.float32
    )
    gate_pre_grad = (
        act_grad * up_pre * sigmoid_val * (1.0 + gate_pre * (1.0 - sigmoid_val))
    ).astype(jnp.bfloat16)
    up_pre_grad = (act_grad * gate_pre * sigmoid_val).astype(jnp.bfloat16)
    gate_grad = lax.dot_general(
        rows_in, gate_pre_grad, contract_rows, preferred_element_type=jnp.float32
    )
    up_grad = lax.dot_general(
        rows_in, up_pre_grad, contract_rows, preferred_element_type=jnp.float32
    )
    input_grad = lax.dot_general(
        gate_pre_grad, gate_mat, contract_cols, preferred_element_type=jnp.float32
    )
    input_grad = input_grad + lax.dot_general(
        up_pre_grad, up_mat, contract_cols, preferred_element_type=jnp.float32
    )
    return (gate_grad, up_grad, down_grad, input_grad)


def compose(higher, nearer):
    return (nearer[0] * higher[0], nearer[1] + nearer[0][:, None, None] * higher[1])


def shards(
    tokens,
    norm_gain,
    cotangent,
    routes,
    route_weight,
    gate_weight,
    up_weight,
    down_weight,
    scan_input,
    out_gate,
    step_size,
    decay_rate,
    write_keys,
    read_keys,
    start_state,
    out_proj,
):
    sp_count = lax.axis_size("sp")
    tp_count = lax.axis_size("tp")
    tok_rows = tokens.shape[0]
    experts_count = sp_count // 2
    capacity = min(tok_rows, 4 * tok_rows // experts_count)
    quarter = D // tp_count
    hidden = tokens.astype(jnp.float32)
    inverse = lax.rsqrt(jnp.mean(hidden * hidden, axis=1) + EPS)
    normed = (hidden * inverse[:, None] * norm_gain[None, :]).astype(jnp.bfloat16)
    route_flat = routes.reshape(-1)
    member = (route_flat[:, None] == jnp.arange(experts_count, dtype=jnp.int32)[None, :]).astype(
        jnp.int32
    )
    earlier_count = jnp.sum((jnp.cumsum(member, axis=0) - member) * member, axis=1)
    places = (route_flat * capacity + earlier_count).reshape(tok_rows, 2)
    slot_ids = jnp.arange(experts_count * capacity, dtype=jnp.int32)[:, None]
    first_hit = slot_ids == places[None, :, 0]
    second_hit = slot_ids == places[None, :, 1]
    placing = jnp.logical_or(first_hit, second_hit)
    place_matrix = placing.astype(jnp.bfloat16)
    slot_weight = jnp.sum(
        jnp.where(first_hit, route_weight[None, :, 0], 0.0)
        + jnp.where(second_hit, route_weight[None, :, 1], 0.0),
        axis=1,
    )
    send_in = jnp.dot(place_matrix, normed, preferred_element_type=jnp.float32).astype(jnp.bfloat16)
    send_cot = (
        slot_weight[:, None] * jnp.dot(place_matrix, cotangent, preferred_element_type=jnp.float32)
    ).astype(jnp.bfloat16)
    half_cap = capacity // 2
    part_in, part_cot = (
        lax.all_to_all(
            send_in.reshape(sp_count, half_cap, D), "sp", split_axis=0, concat_axis=0, tiled=True
        ),
        lax.all_to_all(
            send_cot.reshape(sp_count, half_cap, D), "sp", split_axis=0, concat_axis=0, tiled=True
        ),
    )
    other_in, other_cot = swapped((part_in, part_cot), "sp", 0)
    lower_bit = lax.axis_index("sp") % 2 == 0
    recv_in = jnp.concatenate(
        [jnp.where(lower_bit, part_in, other_in), jnp.where(lower_bit, other_in, part_in)], axis=1
    )
    recv_cot = jnp.concatenate(
        [jnp.where(lower_bit, part_cot, other_cot), jnp.where(lower_bit, other_cot, part_cot)],
        axis=1,
    )
    rows_in = recv_in.reshape(-1, D)
    rows_cot = recv_cot.reshape(-1, D)
    gate_grad, up_grad, down_grad, input_part = expert_grads(
        rows_in, rows_cot, gate_weight[0], up_weight[0], down_weight[0]
    )
    input_quarter = lax.psum_scatter(input_part, "tp", scatter_dimension=1, tiled=True)
    returned = lax.all_to_all(
        input_quarter.reshape(sp_count, capacity, quarter),
        "sp",
        split_axis=0,
        concat_axis=0,
        tiled=True,
    )
    pair_total = jnp.sum(returned.reshape(experts_count, 2, capacity, quarter), axis=1).reshape(
        -1, quarter
    )
    token_quarter = lax.dot_general(
        placing.astype(jnp.float32), pair_total, (((0,), (0,)), ((), ())), precision=HIGHEST
    )
    normed_grad = lax.all_gather(token_quarter, "tp", axis=1, tiled=True)
    gained = norm_gain[None, :] * normed_grad
    dotted = jnp.sum(hidden * gained, axis=1)
    residual = (
        cotangent.astype(jnp.float32)
        + inverse[:, None] * gained
        - hidden * (inverse**3 * dotted / D)[:, None]
    )
    residual_grad = residual.astype(jnp.bfloat16)
    mix_grad = jnp.dot(residual_grad, out_proj, preferred_element_type=jnp.float32)
    per_group = HEADS // GROUPS
    gated, gate_out_grad, decay_now, carried, state_grad = block_forward(
        scan_input,
        out_gate,
        step_size,
        write_keys,
        read_keys,
        decay_rate,
        start_state[0],
        mix_grad,
        per_group,
    )
    totals, later_state = prefix(
        (decay_now, carried), "sp", compose, (jnp.ones_like(decay_now), jnp.zeros_like(carried))
    )
    scan_grad, write_grad, read_grad = block_back(
        scan_input,
        step_size,
        write_keys,
        read_keys,
        decay_rate,
        start_state[0],
        state_grad,
        later_state,
        per_group,
    )
    out_proj_grad = lax.psum_scatter(
        lax.dot_general(
            residual_grad, gated, (((0,), (0,)), ((), ())), preferred_element_type=jnp.float32
        ),
        "sp",
        scatter_dimension=0,
        tiled=True,
    )
    residual_part = lax.dynamic_slice_in_dim(
        residual_grad, lax.axis_index("tp") * quarter, quarter, 1
    )
    return (
        residual_part,
        gate_grad.astype(jnp.bfloat16)[None],
        up_grad.astype(jnp.bfloat16)[None],
        down_grad.astype(jnp.bfloat16)[None],
        out_proj_grad,
        scan_grad,
        gate_out_grad,
        write_grad,
        read_grad,
    )


def moved(value, target):
    sp_count, tp_count = lax.axis_size("sp"), lax.axis_size("tp")
    pairs = []
    for s in range(sp_count):
        for t in range(tp_count):
            to_s, to_t = target(s, t)
            pairs.append((s * tp_count + t, to_s * tp_count + to_t))
    return lax.ppermute(value, ("sp", "tp"), pairs)


def over_core(s, t):
    return s, t ^ 1


def over_y(s, t):
    return s, t ^ 2


def over_x(s, t):
    return s ^ 1, t


def over_z(k):
    return lambda s, t: (s ^ (2 * k), t)


def first_link(s, t):
    return (s ^ 1, t) if t % 2 == 0 else (s, t ^ 2)


def second_link(s, t):
    return (s, t ^ 2) if t % 2 == 0 else (s ^ 1, t)


def ordered(flag, low, high, axis):
    return jnp.concatenate([jnp.where(flag, low, high), jnp.where(flag, high, low)], axis=axis)


def dense_shards(
    tokens,
    norm_gain,
    cotangent,
    routes,
    route_weight,
    gate_weight,
    up_weight,
    down_weight,
    scan_input,
    out_gate,
    step_size,
    decay_rate,
    write_keys,
    read_keys,
    start_state,
    out_proj,
):
    sp_count = lax.axis_size("sp")
    tp_count = lax.axis_size("tp")
    rows, width = tokens.shape
    planes = sp_count // 2
    quarter = width // tp_count
    half = width // 2
    sp_at = lax.axis_index("sp")
    tp_at = lax.axis_index("tp")
    z_at, x_at = sp_at // 2, sp_at % 2
    y_at, c_at = tp_at // 2, tp_at % 2
    x_low, y_low, c_low = x_at == 0, y_at == 0, c_at == 0
    my_quarter = (2 * c_at + y_at) * quarter
    per_group = HEADS // GROUPS

    hidden = tokens.astype(jnp.float32)
    inverse = lax.rsqrt(jnp.mean(hidden * hidden, axis=1) + EPS)
    normed = (hidden * inverse[:, None] * norm_gain[None, :]).astype(jnp.bfloat16)

    def scaled(part, expert):
        weight = jnp.sum(jnp.where(routes == expert, route_weight, 0.0), axis=1)
        return (weight[:, None] * part.astype(jnp.float32)).astype(jnp.bfloat16)

    normed_quarter = lax.dynamic_slice_in_dim(normed, my_quarter, quarter, 1)
    cot_quarter = lax.dynamic_slice_in_dim(cotangent, my_quarter, quarter, 1)

    own_all = jnp.stack([normed, scaled(cotangent, z_at)])
    own_quarter = jnp.stack([normed_quarter, scaled(cot_quarter, z_at)])
    gathered = []
    arrived = {}
    for k in range(1, planes):
        piece = jnp.stack([normed_quarter, scaled(cot_quarter, z_at ^ k)])
        arrived[k] = moved(piece, over_z(k))
    side = moved(own_quarter, over_x)
    side_half = ordered(y_low, side, moved(side, over_y), 2)
    side_all = ordered(c_low, side_half, moved(side_half, over_core), 2)
    gathered.append(jnp.concatenate([own_all, side_all], axis=1))
    for k in range(1, planes):
        mine = arrived[k]
        one = moved(mine, first_link)
        two = moved(mine, second_link)
        both = moved(one, second_link)
        flip_x = jnp.where(c_low, one, two)
        flip_y = jnp.where(c_low, two, one)
        my_half = jnp.concatenate(
            [ordered(y_low, mine, flip_y, 2), ordered(y_low, flip_x, both, 2)], axis=1
        )
        gathered.append(ordered(c_low, my_half, moved(my_half, over_core), 2))
    all_rows = jnp.concatenate(gathered, axis=1)
    gate_grad, up_grad, down_grad, input_part = expert_grads(
        all_rows[0], all_rows[1], gate_weight[0], up_weight[0], down_weight[0]
    )

    part = input_part.reshape(planes, 2, rows, 2, half)
    to_core = jnp.where(c_low, part[..., 1, :], part[..., 0, :]).astype(jnp.bfloat16)
    kept = jnp.where(c_low, part[..., 0, :], part[..., 1, :])
    kept = kept + moved(to_core, over_core).astype(jnp.float32)
    low, high = kept[..., :quarter], kept[..., quarter:]
    same_y = jnp.where(y_low, low, high)
    other_y = jnp.where(y_low, high, low)
    mine, flip_y = same_y[:, 0], other_y[:, 0]
    flip_x, both = same_y[:, 1], other_y[:, 1]
    corner = moved(both.astype(jnp.bfloat16), second_link).astype(jnp.float32)
    one = jnp.where(c_low, flip_x, flip_y) + corner
    two = jnp.where(c_low, flip_y, flip_x)
    mine = (
        mine
        + moved(one.astype(jnp.bfloat16), first_link).astype(jnp.float32)
        + moved(two.astype(jnp.bfloat16), second_link).astype(jnp.float32)
    )
    total = mine[0]
    for k in range(1, planes):
        total = total + moved(mine[k].astype(jnp.bfloat16), over_z(k)).astype(jnp.float32)
    total = total.astype(jnp.bfloat16)
    total_half = ordered(y_low, total, moved(total, over_y), 1)
    total_all = ordered(c_low, total_half, moved(total_half, over_core), 1)

    gained = norm_gain[None, :] * total_all.astype(jnp.float32)
    dotted = jnp.sum(hidden * gained, axis=1)
    residual = (
        cotangent.astype(jnp.float32)
        + inverse[:, None] * gained
        - hidden * (inverse**3 * dotted / width)[:, None]
    )
    residual_grad = residual.astype(jnp.bfloat16)
    mix_grad = jnp.dot(residual_grad, out_proj, preferred_element_type=jnp.float32)
    gated, gate_out_grad, decay_now, carried, state_grad = block_forward(
        scan_input,
        out_gate,
        step_size,
        write_keys,
        read_keys,
        decay_rate,
        start_state[0],
        mix_grad,
        per_group,
    )

    decay_side = moved(decay_now, over_x)
    decay_low = jnp.where(x_low, decay_now, decay_side)
    decay_high = jnp.where(x_low, decay_side, decay_now)
    plane_decay = decay_low * decay_high
    plane_decays = {k: moved(plane_decay, over_z(k)) for k in range(1, planes)}
    carried_side = moved(carried, over_x)
    carry_low = jnp.where(x_low, carried, carried_side)
    carry_high = jnp.where(x_low, carried_side, carried)
    plane_carry = carry_low + decay_low[:, None, None] * carry_high
    above = jnp.zeros_like(carried)
    for k in range(1, planes):
        factor = jnp.where((z_at ^ k) > z_at, jnp.ones_like(decay_now), 0.0)
        for other in range(1, planes):
            if other != k:
                between = ((z_at ^ other) > z_at) & ((z_at ^ other) < (z_at ^ k))
                factor = factor * jnp.where(between, plane_decays[other], 1.0)
        above = above + factor[:, None, None] * moved(plane_carry, over_z(k))
    later_state = jnp.where(x_low, carry_high + decay_high[:, None, None] * above, above)

    scan_grad, write_grad, read_grad = block_back(
        scan_input,
        step_size,
        write_keys,
        read_keys,
        decay_rate,
        start_state[0],
        state_grad,
        later_state,
        per_group,
    )

    columns = width // sp_count
    gated_pair = jnp.stack([gated, moved(gated, over_x)])
    gated_all = [gated_pair] + [moved(gated_pair, over_z(k)) for k in range(1, planes)]

    def columns_for(place):
        return lax.dynamic_slice_in_dim(residual_grad, place * columns, columns, 1)

    to_side = jnp.stack([columns_for(sp_at ^ (2 * k + 1)) for k in range(planes)])
    from_side = moved(to_side, over_x)
    residual_all = []
    for k in range(planes):
        pair = jnp.stack([columns_for(sp_at ^ (2 * k)), from_side[k]])
        residual_all.append(moved(pair, over_z(k)) if k else pair)
    out_proj_grad = lax.dot_general(
        jnp.concatenate(residual_all).reshape(-1, columns),
        jnp.concatenate(gated_all).reshape(-1, gated.shape[1]),
        (((0,), (0,)), ((), ())),
        preferred_element_type=jnp.float32,
    )
    residual_part = lax.dynamic_slice_in_dim(residual_grad, tp_at * quarter, quarter, 1)
    return (
        residual_part,
        gate_grad.astype(jnp.bfloat16)[None],
        up_grad.astype(jnp.bfloat16)[None],
        down_grad.astype(jnp.bfloat16)[None],
        out_proj_grad,
        scan_grad,
        gate_out_grad,
        write_grad,
        read_grad,
    )


def local_body(mesh):
    sp_count, tp_count = mesh.shape["sp"], mesh.shape["tp"]
    experts = sp_count // 2

    def body(tokens, *rest):
        rows = tokens.shape[0]
        power = experts & (experts - 1) == 0
        if tp_count == 4 and power and 4 * rows // experts >= rows:
            return dense_shards(tokens, *rest)
        return shards(tokens, *rest)

    return body


def solution(mesh):
    return jax.shard_map(
        local_body(mesh),
        mesh=mesh,
        in_specs=(
            P("sp", None),
            P(),
            P("sp", None),
            P("sp", None),
            P("sp", None),
            P("sp", None, "tp"),
            P("sp", None, "tp"),
            P("sp", "tp", None),
            P("sp", "tp"),
            P("sp", "tp"),
            P("tp", "sp"),
            P("tp"),
            P("sp", "tp"),
            P("sp", "tp"),
            P("sp", "tp", None, None),
            P(None, "tp"),
        ),
        out_specs=(
            P("sp", "tp"),
            P("sp", None, "tp"),
            P("sp", None, "tp"),
            P("sp", "tp", None),
            P("sp", "tp"),
            P("sp", "tp"),
            P("sp", "tp"),
            P("sp", "tp"),
            P("sp", "tp"),
        ),
        check_vma=False,
    )
```
